32 devices in a mesh: sp: 8 (over z, x), tp: 4 (over y, core).
Axes of the slice: x: 2, y: 2, z: 4, core: 2. Of those that a mesh axis runs over, the one named last changes fastest.
Arguments:
- queries: bfloat16 [1024, 2048], P('sp', 'tp'), may hold values from -18 to 90
- projected_key_rows: bfloat16 [1024, 1024], P('sp', 'tp'), may hold values from -18 to 90
- projected_value_rows: bfloat16 [1024, 1024], P('sp', 'tp'), may hold values from -6 to 6
- query_gain: float32 [64], replicated, may hold values from 1 to 6
- key_norm_gain: float32 [64], replicated, may hold values from 1 to 6
- residual: bfloat16 [1024, 2048], P('sp', 'tp'), may hold values from -54 to 54
- out_weight: bfloat16 [2048, 2048], P('tp'), may hold values from -1 to 1
- norm_gain: float32 [2048], P('tp'), may hold values from 0.28 to 4.68
- expert_ids: int32 [1024, 2], P('sp'), may hold values from 0 to 7, as said below
- route_weights: float32 [1024, 2], P('sp'), may hold values from 0.2 to 1
- gate_weight: bfloat16 [8, 2048, 4096], P('sp', None, 'tp'), may hold values from -0.125 to 0.125
- up_weight: bfloat16 [8, 2048, 4096], P('sp', None, 'tp'), may hold values from -0.125 to 0.125
- down_weight: bfloat16 [8, 4096, 2048], P('sp', 'tp'), may hold values from -0.25 to 0.25
- final_gain: float32 [2048], P('tp'), may hold values from 0.1 to 1.9
Outputs:
- layer_out: bfloat16 [1024, 2048], P('sp', 'tp')
The draws below stay inside these ranges and needn't reach their ends.
Inputs may be any that keep to these rules, and one draw needn't show every extreme that they name: `expert_ids`: each row names two different experts of one group, the group of expert e being e // 4. In every aligned block of 128 rows each group is named by the same number of rows, no expert is named by more than 64 rows, one expert of every group is named by exactly 64 rows, and one expert is named by 64 rows of every block.
All inputs are finite; a program needn't handle non-finite values.
Results may differ from the reference program's by a relative error of at most 0.019.
The reference program's roundings to bfloat16 on the way count: a program that leaves them out, or rounds other values in their place, can miss the bound.
Values may be sent and summed in bfloat16 or wider, within the bound.
A program may use at most 64 MiB of HBM per device.

```python
import jax
import jax.numpy as jnp
from jax import lax

D = 2048
QUERY_HEAD_COUNT = 32
KEY_VALUE_HEADS = 16
HEAD_DIM = 64
GRID_W = 64
FFE = 4096
EXP_GROUP = 4
TOPK = 2
TOK_SP = 128
SEQUENCE_TOKENS = 1024
EXPERTS = 8
CAP = 64
UNIT_BLOCKS = 4


def draw_rows_by_head(key, head_count):
    normal_part = jnp.clip(jax.random.normal(jax.random.fold_in(key, 1), (SEQUENCE_TOKENS, head_count, HEAD_DIM), jnp.float32), -6.0, 6.0)
    return normal_part.reshape(SEQUENCE_TOKENS, head_count * HEAD_DIM)


def draw_queries(key, part):
    return draw_rows_by_head(jax.random.fold_in(key, 101), QUERY_HEAD_COUNT).astype(jnp.bfloat16)


def draw_projected_key_rows(key, part):
    return draw_rows_by_head(jax.random.fold_in(key, 102), KEY_VALUE_HEADS).astype(jnp.bfloat16)


def draw_gain_row(key):
    base_gain = jax.random.uniform(jax.random.fold_in(key, 1), (HEAD_DIM,), jnp.float32, 1.0, 1.8)
    return base_gain


def draw_query_gain(key, part):
    return draw_gain_row(jax.random.fold_in(key, 103))


def draw_key_norm_gain(key, part):
    return draw_gain_row(jax.random.fold_in(key, 104))


def draw_residual(key, part):
    normal_part = jnp.clip(jax.random.normal(jax.random.fold_in(key, 105), (SEQUENCE_TOKENS, D), jnp.float32), -6.0, 6.0)
    columns = jnp.arange(D, dtype=jnp.float32) / D
    return (normal_part * 0.5 * 3.0 ** columns[None, :]).astype(jnp.bfloat16)


def draw_norm_gain(key, part):
    base_gain = jax.random.uniform(jax.random.fold_in(key, 107), (D,), jnp.float32, 0.7, 1.3)
    columns = jnp.arange(D, dtype=jnp.float32) / D
    return base_gain * 0.6 * 3.0 ** columns


def draw_expert_ids(key, part):
    block_count = SEQUENCE_TOKENS // TOK_SP
    group_count = EXPERTS // EXP_GROUP
    group_rows = TOK_SP // group_count
    mean_load = 2 * group_rows // EXP_GROUP
    hot_first = jax.random.randint(jax.random.fold_in(key, 21), (), 0, EXP_GROUP)
    lane_index = jnp.arange(EXP_GROUP, dtype=jnp.int32)
    list_index = jnp.arange(2 * group_rows, dtype=jnp.int32)

    def one_group(group_key, group_number):
        heights = jax.random.randint(group_key, (EXP_GROUP,), 0, mean_load + 1)
        peak_at = jax.random.randint(jax.random.fold_in(group_key, 1), (), 0, EXP_GROUP)
        peak_at = jnp.where(group_number == 0, hot_first, peak_at)
        heights = jnp.where(lane_index == peak_at, mean_load, heights)
        heights = jnp.where(lane_index == (peak_at + EXP_GROUP - 1) % EXP_GROUP, 0, heights)
        loads = mean_load + heights - jnp.roll(heights, 1)
        ends = jnp.cumsum(loads)
        listing = jnp.sum((ends[None, :] <= list_index[:, None]).astype(jnp.int32), 1)
        return jnp.stack([listing[:group_rows], listing[group_rows:]], 1) + group_number * EXP_GROUP

    def one_block(block_key):
        group_keys = jax.random.split(block_key, group_count)
        pairs = jax.vmap(one_group)(group_keys, jnp.arange(group_count, dtype=jnp.int32)).reshape(TOK_SP, TOPK)
        order = jax.random.permutation(jax.random.fold_in(block_key, 7), TOK_SP)
        pairs = pairs[order]
        flipped = jax.random.randint(jax.random.fold_in(block_key, 8), (TOK_SP, 1), 0, 2)
        return jnp.where(flipped == 1, pairs[:, ::-1], pairs)
    block_keys = jax.random.split(jax.random.fold_in(key, 20), block_count)
    return jax.vmap(one_block)(block_keys).reshape(SEQUENCE_TOKENS, TOPK).astype(jnp.int32)


def raised(array, own_key, source, target, shards_of, factor):
    owner, partner = [(jnp.arange(array.shape[axis_at]) // (array.shape[axis_at] // shards_of)).reshape([-1 if axis == axis_at else 1 for axis in range(array.ndim)]) for axis_at in (source, target)]
    chosen = jax.random.permutation(own_key, shards_of)[partner]
    strong = (owner == chosen) | (owner == (partner + shards_of // 2) % shards_of)
    return jnp.where(strong, factor * array, array)


def levels(stream_key, extent, cuts, low, top_value):
    gain, own = 1.0, jax.random.fold_in(stream_key, 6)
    for axis_at, shards_of in cuts:
        steps = jnp.exp(jax.random.uniform(jax.random.fold_in(own, axis_at), (shards_of,), jnp.float32, low / len(cuts), top_value / len(cuts)))
        gain = gain * jnp.repeat(steps, extent[axis_at] // shards_of).reshape([-1 if axis == axis_at else 1 for axis in range(len(extent))])
    return gain


def normal_values(own_key, shape, width, most, cuts=(), kind=jnp.bfloat16):
    array = jax.random.normal(own_key, shape, jnp.float32) * width
    if len(cuts) > 0:
        array = levels(own_key, shape, cuts, -0.22, 0.18) * array
    return jnp.clip(array, min=-most, max=most).astype(kind)


def gaussian_with(own_key, dims, deviation, bound, shards, heavy, kind=jnp.bfloat16):
    entries = deviation * jax.random.normal(own_key, dims, jnp.float32)
    if shards:
        entries = entries * levels(own_key, dims, shards, -0.22, 0.18)
    return jnp.clip(raised(entries, jax.random.fold_in(own_key, 3), *heavy), -bound, bound).astype(kind)


def setup_inputs(seed: int = 0) -> dict:
    key_of = jax.random.split(jax.random.key(seed), 15)
    queries = draw_queries(jax.random.fold_in(key_of[14], 71), 0)
    projected_key_rows = draw_projected_key_rows(jax.random.fold_in(key_of[14], 71), 0)
    projected_value_rows = normal_values(key_of[2], (SEQUENCE_TOKENS, KEY_VALUE_HEADS * HEAD_DIM), 1.0, 6.0, ((0, 8), (1, 4)))
    query_gain = draw_query_gain(jax.random.fold_in(key_of[14], 71), 0)
    key_norm_gain = draw_key_norm_gain(jax.random.fold_in(key_of[14], 71), 0)
    residual = draw_residual(jax.random.fold_in(key_of[14], 71), 0)
    out_weight = gaussian_with(key_of[6], (QUERY_HEAD_COUNT * HEAD_DIM, D), (QUERY_HEAD_COUNT * HEAD_DIM // 32) ** -0.5, 1.0, ((0, 4),), (0, 1, 4, 2.0))
    norm_gain = draw_norm_gain(jax.random.fold_in(key_of[14], 71), 0)
    expert_ids = draw_expert_ids(jax.random.fold_in(key_of[14], 71), 0)
    route_weights = jnp.clip(0.2 + 0.8 * jax.random.uniform(key_of[9], (SEQUENCE_TOKENS, TOPK), jnp.float32) ** levels(key_of[9], (SEQUENCE_TOKENS, TOPK), ((0, 8),), -0.2, 0.2), 0.2, 1.0)
    gate_weight = normal_values(key_of[10], (EXPERTS, D, FFE), D ** -0.5, 0.125, ((0, 8), (2, 4)))
    up_weight = normal_values(key_of[11], (EXPERTS, D, FFE), D ** -0.5, 0.125, ((0, 8), (2, 4)))
    down_weight = gaussian_with(key_of[12], (EXPERTS, FFE, D), (FFE // 4) ** -0.5, 0.25, ((0, 8), (1, 4)), (1, 2, 4, 2.0))
    final_gain = jnp.clip(1.0 + 0.18 * jax.random.normal(key_of[13], (D,), jnp.float32), 0.1, 1.9)
    return dict(queries=queries, projected_key_rows=projected_key_rows, projected_value_rows=projected_value_rows, query_gain=query_gain, key_norm_gain=key_norm_gain, residual=residual, out_weight=out_weight, norm_gain=norm_gain, expert_ids=expert_ids, route_weights=route_weights, gate_weight=gate_weight, up_weight=up_weight, down_weight=down_weight, final_gain=final_gain)


theta_base = 10000.0
norm_epsilon = 1e-06
residual_scale = 8.0 ** 0.25

def rope_line(halves, angles):
    pair_count = angles.shape[-1]
    first_half = halves[..., :pair_count]
    second_half = halves[..., pair_count:]
    cosine = jnp.cos(angles)[:, None, :]
    sine_part = jnp.sin(angles)[:, None, :]
    return jnp.concatenate([first_half * cosine - second_half * sine_part, first_half * sine_part + second_half * cosine], -1)

def rotary_over_grid(rows_by_head, token_positions):
    head_size = rows_by_head.shape[-1]
    frequency = theta_base ** (-jnp.arange(0, head_size // 2, 2, dtype=jnp.float32) / (head_size // 2))
    grid_row = (token_positions // GRID_W).astype(jnp.float32)
    grid_col = (token_positions % GRID_W).astype(jnp.float32)
    row_part = rope_line(rows_by_head[..., :head_size // 2], grid_row[:, None] * frequency[None, :])
    col_part = rope_line(rows_by_head[..., head_size // 2:], grid_col[:, None] * frequency[None, :])
    return jnp.concatenate([row_part, col_part], -1)

def normalize_heads(token_rows, gain_row, head_count):
    shaped = token_rows.astype(jnp.float32).reshape(token_rows.shape[0], head_count, -1)
    scaled = shaped * lax.rsqrt(lax.optimization_barrier(jnp.mean(shaped * shaped, -1, keepdims=True)) + norm_epsilon)
    return scaled * gain_row[None, None, :]

def layer_norm(stream):
    center = lax.optimization_barrier(jnp.mean(stream, -1, keepdims=True))
    spread = lax.optimization_barrier(jnp.mean(jnp.square(stream - center), -1, keepdims=True))
    return (stream - center) * lax.rsqrt(spread + norm_epsilon)

def attend_group(operands):
    head_queries, head_keys, head_values = operands
    scores = jnp.einsum('gqd,kd->gqk', head_queries.astype(jnp.float32), head_keys.astype(jnp.float32)) * HEAD_DIM ** (-0.5)
    weights = jnp.exp(scores - lax.optimization_barrier(jnp.max(scores, -1, keepdims=True)))
    row_total = lax.optimization_barrier(jnp.sum(weights, -1, keepdims=True))
    rounded = lax.optimization_barrier(weights.astype(jnp.bfloat16)).astype(jnp.float32)
    gathered = jnp.einsum('gqk,kd->gqd', rounded, head_values.astype(jnp.float32))
    return (gathered / row_total).astype(jnp.bfloat16)

def block_slots(block_ids):
    onehot = (block_ids[:, None] == jnp.arange(EXPERTS, dtype=jnp.int32)[None, :]).astype(jnp.int32)
    earlier = jnp.cumsum(onehot, 0) - onehot
    return lax.optimization_barrier(jnp.sum(earlier * onehot, 1))

def expert_rows(operands):
    token_rows, gate_mat, up_mat, down_mat = operands
    gate_sum = jnp.dot(token_rows, gate_mat, preferred_element_type=jnp.float32)
    up_sum = jnp.dot(token_rows, up_mat, preferred_element_type=jnp.float32)
    hidden = (jax.nn.silu(gate_sum) * up_sum).astype(jnp.bfloat16)
    split_hidden = hidden.reshape(hidden.shape[0], UNIT_BLOCKS, -1).astype(jnp.float32)
    split_down = down_mat.reshape(UNIT_BLOCKS, -1, down_mat.shape[-1]).astype(jnp.float32)
    partial_sums = jnp.einsum('rtf,tfd->trd', split_hidden, split_down)
    rounded = lax.optimization_barrier(partial_sums.astype(jnp.bfloat16)).astype(jnp.float32)
    return lax.optimization_barrier(jnp.sum(rounded, 0)).astype(jnp.bfloat16)

def reference(queries, projected_key_rows, projected_value_rows, query_gain, key_norm_gain, residual, out_weight, norm_gain, expert_ids, route_weights, gate_weight, up_weight, down_weight, final_gain):
    token_positions = jnp.arange(SEQUENCE_TOKENS, dtype=jnp.int32)
    queries_per_group = QUERY_HEAD_COUNT // KEY_VALUE_HEADS
    queries_after_rotation = rotary_over_grid(normalize_heads(queries, query_gain, QUERY_HEAD_COUNT), token_positions).astype(jnp.bfloat16)
    keys_after_rotation = rotary_over_grid(normalize_heads(projected_key_rows, key_norm_gain, KEY_VALUE_HEADS), token_positions).astype(jnp.bfloat16)
    grouped_query_heads = queries_after_rotation.reshape(SEQUENCE_TOKENS, KEY_VALUE_HEADS, queries_per_group, HEAD_DIM).transpose(1, 2, 0, 3)
    key_heads = keys_after_rotation.transpose(1, 0, 2)
    value_per_head = projected_value_rows.reshape(SEQUENCE_TOKENS, KEY_VALUE_HEADS, HEAD_DIM).transpose(1, 0, 2)
    attended = lax.map(attend_group, (grouped_query_heads, key_heads, value_per_head))
    attended = attended.transpose(2, 0, 1, 3).reshape(SEQUENCE_TOKENS, QUERY_HEAD_COUNT * HEAD_DIM)
    mixed_rows = jnp.dot(attended, out_weight, preferred_element_type=jnp.float32)
    pre_norm = residual_scale * residual.astype(jnp.float32) + mixed_rows
    normed = (layer_norm(pre_norm) * norm_gain[None, :]).astype(jnp.bfloat16)
    block_count = SEQUENCE_TOKENS // TOK_SP
    slots = jax.vmap(block_slots)(expert_ids.reshape(block_count, TOK_SP * TOPK)).reshape(SEQUENCE_TOKENS, TOPK)
    blocks = (jnp.arange(SEQUENCE_TOKENS, dtype=jnp.int32) // TOK_SP)[:, None]
    places = expert_ids * (block_count * CAP) + blocks * CAP + slots
    routed = jnp.zeros((EXPERTS * block_count * CAP, D), jnp.bfloat16)
    routed = routed.at[places.reshape(-1)].set(jnp.repeat(normed, TOPK, axis=0))
    expert_out = lax.map(expert_rows, (routed.reshape(EXPERTS, block_count * CAP, D), gate_weight, up_weight, down_weight))
    flat_out = expert_out.reshape(-1, D)
    combined = jnp.zeros((SEQUENCE_TOKENS, D), jnp.float32)
    for route_rank in range(TOPK):
        combined = combined + route_weights[:, route_rank:route_rank + 1] * flat_out[places[:, route_rank]].astype(jnp.float32)
    second_sum = residual_scale * normed.astype(jnp.float32) + combined
    return (layer_norm(second_sum) * final_gain[None, :]).astype(jnp.bfloat16)
```

```python
import jax
import jax.numpy as jnp
from jax import lax
from jax.experimental import pallas as pl
from jax.experimental.pallas import tpu as pltpu
from jax.sharding import PartitionSpec as P

D = 2048
HEAD_DIM = 64
GRID_W = 64
TOPK = 2


theta_base = 10000.0
norm_epsilon = 1e-06
residual_scale = 8.0**0.25
far_below = -1e30
MESH = pl.DeviceIdType.MESH


def rope_line(halves, angles):
    pair_count = angles.shape[-1]
    first_half = halves[..., :pair_count]
    second_half = halves[..., pair_count:]
    cosine = jnp.cos(angles)[:, None, :]
    sine_part = jnp.sin(angles)[:, None, :]
    return jnp.concatenate(
        [
            first_half * cosine - second_half * sine_part,
            first_half * sine_part + second_half * cosine,
        ],
        -1,
    )


def rotary_over_grid(rows_by_head, token_positions):
    head_size = rows_by_head.shape[-1]
    frequency = theta_base ** (
        -jnp.arange(0, head_size // 2, 2, dtype=jnp.float32) / (head_size // 2)
    )
    grid_row = (token_positions // GRID_W).astype(jnp.float32)
    grid_col = (token_positions % GRID_W).astype(jnp.float32)
    row_part = rope_line(
        rows_by_head[..., : head_size // 2], grid_row[:, None] * frequency[None, :]
    )
    col_part = rope_line(
        rows_by_head[..., head_size // 2 :], grid_col[:, None] * frequency[None, :]
    )
    return jnp.concatenate([row_part, col_part], -1)


def normalize_heads(token_rows, gain_row, head_count):
    shaped = token_rows.astype(jnp.float32).reshape(token_rows.shape[0], head_count, -1)
    scaled = shaped * lax.rsqrt(jnp.mean(shaped * shaped, -1, keepdims=True) + norm_epsilon)
    return scaled * gain_row[None, None, :]


def ring_gather(packed, group, group_minor):
    rows, width = packed.shape
    pieces = 4
    piece = rows // pieces
    half = group // 2
    major = group // group_minor

    def place_of(index):
        high, low = index // group_minor, lax.rem(index, group_minor)
        if group_minor == 1:
            return high
        back = major - 1 - high
        odd = lax.rem(back, 2)
        inner = (low - 1) * (1 - odd) + (group_minor - 1 - low) * odd
        first = jnp.where(low == 0, 1, 0)
        return first * high + (1 - first) * (major + back * (group_minor - 1) + inner)

    def device_at(place):
        if group_minor == 1:
            return place
        first = jnp.where(place < major, 1, 0)
        rest = jnp.maximum(place - major, 0)
        back = rest // (group_minor - 1)
        inner = lax.rem(rest, group_minor - 1)
        odd = lax.rem(back, 2)
        low = 1 + inner * (1 - odd) + (group_minor - 2 - inner) * odd
        other = (major - 1 - back) * group_minor + low
        return first * (place * group_minor) + (1 - first) * other

    def kernel(mine_ref, all_ref, send_sem, recv_sem, own_sem):
        me = lax.axis_index("sp")
        spot = place_of(me)
        right = device_at(lax.rem(spot + 1, group))
        left = device_at(lax.rem(spot + group - 1, group))
        barrier = pltpu.get_barrier_semaphore()
        for neighbour in (left, right):
            pl.semaphore_signal(
                barrier, inc=1, device_id={"sp": neighbour}, device_id_type=MESH
            )
        pl.semaphore_wait(barrier, 2)
        own = pltpu.make_async_copy(mine_ref, all_ref.at[0], own_sem)
        own.start()
        copies = {}
        for hop in range(1, half + 1):
            for part in range(pieces):
                span = pl.ds(part * piece, piece)
                for way in range(2):
                    if hop == half and (part < pieces // 2) != (way == 0):
                        continue
                    if hop > 1:
                        copies[way, hop - 1, part].wait_recv()
                    source_slot = (hop - 1) if way == 0 else (group - hop + 1)
                    target_slot = hop if way == 0 else group - hop
                    source = mine_ref.at[span] if hop == 1 else all_ref.at[source_slot, span]
                    copy = pltpu.make_async_remote_copy(
                        src_ref=source,
                        dst_ref=all_ref.at[target_slot, span],
                        send_sem=send_sem.at[way, hop - 1, part],
                        recv_sem=recv_sem.at[way, hop - 1, part],
                        device_id={"sp": right if way == 0 else left},
                        device_id_type=MESH,
                    )
                    copy.start()
                    copies[way, hop, part] = copy
        for way, hop, part in copies:
            if hop == half or (hop == half - 1 and (way, half, part) not in copies):
                copies[way, hop, part].wait_recv()
        for copy in copies.values():
            copy.wait_send()
        own.wait()

    return pl.pallas_call(
        kernel,
        out_shape=jax.ShapeDtypeStruct((group, rows, width), packed.dtype),
        in_specs=[pl.BlockSpec(memory_space=pltpu.VMEM)],
        out_specs=pl.BlockSpec(memory_space=pltpu.VMEM),
        scratch_shapes=[
            pltpu.SemaphoreType.DMA((2, half, pieces)),
            pltpu.SemaphoreType.DMA((2, half, pieces)),
            pltpu.SemaphoreType.DMA,
        ],
        compiler_params=pltpu.CompilerParams(
            collective_id=0, has_side_effects=True, vmem_limit_bytes=24 << 20
        ),
    )(packed)


def after_attention(
    attended, out_weight, residual, norm_gain, places, route_weights, gate_weight, up_weight,
    down_weight, final_gain, experts, shards,
):
    token_count, width = residual.shape
    lines = shards // 2
    row_total = TOPK * 2 * token_count
    capacity = row_total // experts
    groups = 4
    group_rows = row_total // groups
    group_experts = experts // groups
    halves = 2
    half_rows = row_total // halves
    hidden_units = gate_weight.shape[2]
    tile = min(256, hidden_units)
    feature_total = width * shards
    places_across = places.T
    bf16, f32 = jnp.bfloat16, jnp.float32

    def kernel(
        att_ref, ow_ref, res_ref, gain_ref, at_ref, across_ref, rw_ref, gate_hbm, up_hbm, down_hbm,
        last_gain_ref, out_ref,
        gate_v, up_v, down_v, weight_sem,
        mix_send, mix_pair, line_send, line_recv, mix_sem, line_sem,
        stat_send, stat_recv, stat_sem,
        outgoing, routed, out_sem, fwd_sem, cross_sem, relay_sem,
        hidden, part_send, part_pair, sum_send, sum_recv, own_sum, part_sem, sum_sem,
        result, returned, back_sem,
    ):
        me_s = lax.axis_index("sp")
        me_t = lax.axis_index("tp")
        line = me_t // 2
        core = lax.rem(me_t, 2)
        partner = line * 2 + 1 - core

        def line_at(step):
            return lax.rem(line + step, lines)

        barrier = pltpu.get_barrier_semaphore()
        for step in range(1, experts):
            pl.semaphore_signal(
                barrier, inc=1, device_id={"sp": lax.rem(me_s + step, experts)},
                device_id_type=MESH,
            )
        for step in range(1, shards):
            pl.semaphore_signal(
                barrier, inc=1, device_id={"tp": lax.rem(me_t + step, shards)},
                device_id_type=MESH,
            )
        loads = [
            pltpu.make_async_copy(src.at[0], dst, weight_sem.at[i])
            for i, (src, dst) in enumerate(
                ((gate_hbm, gate_v), (up_hbm, up_v), (down_hbm, down_v))
            )
        ]
        for load in loads:
            load.start()
        sent = []

        def push(source, target, sems, index, device):
            copy = pltpu.make_async_remote_copy(
                src_ref=source, dst_ref=target,
                send_sem=sems.at[(0,) + index], recv_sem=sems.at[(1,) + index],
                device_id=device, device_id_type=MESH,
            )
            copy.start()
            sent.append(copy)
            return copy

        attended_rows = att_ref[...]

        def mix(shard):
            return jnp.dot(
                attended_rows,
                ow_ref[:, pl.ds(pl.multiple_of(shard * width, width), width)],
                preferred_element_type=f32,
            )

        for step in range(lines):
            mix_send[step] = mix(line_at(step) * 2 + 1 - core).astype(bf16)
        pl.semaphore_wait(barrier, experts + shards - 2)
        pair = {}
        for step in list(range(1, lines)) + [0]:
            pair[step] = push(
                mix_send.at[step], mix_pair.at[step], mix_sem, (step,), {"tp": partner}
            )
        across = {}
        for step in range(1, lines):
            mine = mix(line_at(step) * 2 + core)
            pair[step].wait_recv()
            line_send[step - 1] = (mine + mix_pair[step].astype(f32)).astype(bf16)
            across[step] = push(
                line_send.at[step - 1], line_recv.at[step - 1], line_sem, (step - 1,),
                {"tp": line_at(step) * 2 + core},
            )
        total = mix(me_t)
        pair[0].wait_recv()
        total = total + mix_pair[0].astype(f32)
        total = total + residual_scale * res_ref[...].astype(f32)
        for step in range(1, lines):
            across[step].wait_recv()
            total = total + line_recv[step - 1].astype(f32)

        lane = lax.broadcasted_iota(jnp.int32, (token_count, 128), 1)

        def normalize(values, gain, turn):
            sums = jnp.sum(values, 1, keepdims=True)
            squares = jnp.sum(values * values, 1, keepdims=True)
            both = jnp.where(lane == 0, sums, jnp.where(lane == 1, squares, 0.0)).T[:8]
            stat_send[turn] = both
            stats = [
                push(
                    stat_send.at[turn], stat_recv.at[turn, step - 1], stat_sem,
                    (turn, step - 1), {"tp": lax.rem(me_t + step, shards)},
                )
                for step in range(1, shards)
            ]
            for step in range(1, shards):
                stats[step - 1].wait_recv()
                both = both + stat_recv[turn, step - 1]
            columns = jnp.concatenate([both] * 16, 0).T
            center = columns[:, 0:1] / feature_total
            spread = columns[:, 1:2] / feature_total - center * center
            return (values - center) * lax.rsqrt(spread + norm_epsilon) * gain

        normed = normalize(total, gain_ref[...], 0).astype(bf16)
        row_index = lax.broadcasted_iota(jnp.int32, (row_total, token_count), 0)
        picks = jnp.where(
            (row_index == across_ref[0:1, :]) | (row_index == across_ref[1:2, :]), 1.0, 0.0
        ).astype(bf16)
        spread_rows = jnp.dot(picks, normed, preferred_element_type=f32).astype(bf16)
        outgoing[...] = spread_rows
        routed[me_t, pl.ds(0, capacity)] = spread_rows[:capacity]
        arrivals = {}
        for step in range(1, experts):
            rows = pl.ds(step * capacity, capacity)
            arrivals[step] = push(
                outgoing.at[rows], routed.at[me_t, rows], out_sem, (step,),
                {"sp": lax.rem(me_s + step, experts)},
            )
        forwards, crossings, relays = {}, {}, {}

        def forward(group):
            for step in range(group * group_experts, (group + 1) * group_experts):
                if step > 0:
                    arrivals[step].wait_recv()
            rows = pl.ds(group * group_rows, group_rows)
            block = routed.at[me_t, rows]
            for step in range(1, lines):
                crossings[group, step] = push(
                    block, block, cross_sem, (group, step - 1),
                    {"tp": line_at(step) * 2 + core},
                )
            forwards[group] = push(block, block, fwd_sem, (group,), {"tp": partner})

        def relay(group):
            rows = pl.ds(group * group_rows, group_rows)
            for step in range(1, lines):
                crossings[group, step].wait_recv()
                block = routed.at[line_at(lines - step) * 2 + core, rows]
                relays[group, step] = push(
                    block, block, relay_sem, (group, step - 1), {"tp": partner}
                )

        def settle(group):
            forwards[group].wait_recv()
            for step in range(1, lines):
                relays[group, step].wait_recv()

        def expand(half):
            rows = pl.ds(half * half_rows, half_rows)

            def one_tile(index, carry):
                cols = pl.ds(pl.multiple_of(index * tile, tile), tile)
                gate_sum = jnp.zeros((half_rows, tile), f32)
                up_sum = jnp.zeros((half_rows, tile), f32)
                for shard in range(shards):
                    block = routed[shard, rows]
                    deep = pl.ds(shard * width, width)
                    gate_sum += jnp.dot(block, gate_v[deep, cols], preferred_element_type=f32)
                    up_sum += jnp.dot(block, up_v[deep, cols], preferred_element_type=f32)
                hidden[rows, cols] = (
                    gate_sum / (1.0 + jnp.exp(-gate_sum)) * up_sum
                ).astype(bf16)
                return carry

            lax.fori_loop(0, hidden_units // tile, one_tile, 0)

        def down(half, shard):
            return jnp.dot(
                hidden[pl.ds(half * half_rows, half_rows)],
                down_v[:, pl.ds(pl.multiple_of(shard * width, width), width)],
                preferred_element_type=f32,
            )

        parts, sums = {}, {}

        def shrink(half):
            for step in list(range(1, lines)) + [0]:
                part_send[half, step] = down(half, line_at(step) * 2 + 1 - core).astype(bf16)
                parts[half, step] = push(
                    part_send.at[half, step], part_pair.at[half, step], part_sem, (half, step),
                    {"tp": partner},
                )
            for step in range(1, lines):
                mine = down(half, line_at(step) * 2 + core)
                parts[half, step].wait_recv()
                sum_send[half, step - 1] = (
                    mine + part_pair[half, step].astype(f32)
                ).astype(bf16)
                sums[half, step] = push(
                    sum_send.at[half, step - 1], sum_recv.at[half, step - 1], sum_sem,
                    (half, step - 1), {"tp": line_at(step) * 2 + core},
                )
            own_sum[half] = down(half, me_t)

        backs = {}

        def finish(half):
            parts[half, 0].wait_recv()
            value = own_sum[half] + part_pair[half, 0].astype(f32)
            for step in range(1, lines):
                sums[half, step].wait_recv()
                value = value + sum_recv[half, step - 1].astype(f32)
            value = value.astype(bf16)
            result[pl.ds(half * half_rows, half_rows)] = value
            first = half * (experts // halves)
            if half == 0:
                returned[pl.ds(0, capacity)] = value[:capacity]
            for step in range(max(first, 1), first + experts // halves):
                rows = pl.ds(step * capacity, capacity)
                backs[step] = push(
                    result.at[rows], returned.at[rows], back_sem, (step,),
                    {"sp": lax.rem(me_s + experts - step, experts)},
                )

        forward(0)
        forward(1)
        relay(0)
        forward(2)
        relay(1)
        forward(3)
        for load in loads[:2]:
            load.wait()
        settle(0)
        settle(1)
        expand(0)
        relay(2)
        loads[2].wait()
        shrink(0)
        relay(3)
        settle(2)
        settle(3)
        expand(1)
        finish(0)
        shrink(1)
        finish(1)
        slot_index = lax.broadcasted_iota(jnp.int32, (token_count, row_total), 1)
        choose = [
            jnp.where(slot_index == at_ref[:, k : k + 1], 1.0, 0.0).astype(bf16)
            for k in range(TOPK)
        ]
        for step in range(1, experts):
            backs[step].wait_recv()
        second_sum = residual_scale * normed.astype(f32)
        back_rows = returned[...]
        for k in range(TOPK):
            second_sum = second_sum + rw_ref[:, k : k + 1] * jnp.dot(
                choose[k], back_rows, preferred_element_type=f32
            )
        out_ref[...] = normalize(second_sum, last_gain_ref[...], 1).astype(bf16)
        for copy in sent:
            copy.wait_send()

    vmem = pl.BlockSpec(memory_space=pltpu.VMEM)
    hbm = pl.BlockSpec(memory_space=pl.ANY)
    dma = pltpu.SemaphoreType.DMA
    other = max(lines - 1, 1)
    return pl.pallas_call(
        kernel,
        out_shape=jax.ShapeDtypeStruct((token_count, width), bf16),
        in_specs=[vmem] * 7 + [hbm] * 3 + [vmem],
        out_specs=vmem,
        scratch_shapes=[
            pltpu.VMEM(gate_weight.shape[1:], bf16),
            pltpu.VMEM(up_weight.shape[1:], bf16),
            pltpu.VMEM(down_weight.shape[1:], bf16),
            dma((3,)),
            pltpu.VMEM((lines, token_count, width), bf16),
            pltpu.VMEM((lines, token_count, width), bf16),
            pltpu.VMEM((other, token_count, width), bf16),
            pltpu.VMEM((other, token_count, width), bf16),
            dma((2, lines)),
            dma((2, other)),
            pltpu.VMEM((2, 8, token_count), f32),
            pltpu.VMEM((2, shards - 1, 8, token_count), f32),
            dma((2, 2, shards - 1)),
            pltpu.VMEM((row_total, width), bf16),
            pltpu.VMEM((shards, row_total, width), bf16),
            dma((2, experts)),
            dma((2, groups)),
            dma((2, groups, other)),
            dma((2, groups, other)),
            pltpu.VMEM((row_total, hidden_units), bf16),
            pltpu.VMEM((halves, lines, half_rows, width), bf16),
            pltpu.VMEM((halves, lines, half_rows, width), bf16),
            pltpu.VMEM((halves, other, half_rows, width), bf16),
            pltpu.VMEM((halves, other, half_rows, width), bf16),
            pltpu.VMEM((halves, half_rows, width), f32),
            dma((2, halves, lines)),
            dma((2, halves, other)),
            pltpu.VMEM((row_total, width), bf16),
            pltpu.VMEM((row_total, width), bf16),
            dma((2, experts)),
        ],
        compiler_params=pltpu.CompilerParams(
            collective_id=1, has_side_effects=True, vmem_limit_bytes=50 << 20
        ),
    )(
        attended, out_weight, residual, norm_gain.reshape(1, -1), places, places_across,
        route_weights, gate_weight, up_weight, down_weight, final_gain.reshape(1, -1),
    )


def per_device(
    queries,
    projected_key_rows,
    projected_value_rows,
    query_gain,
    key_norm_gain,
    residual,
    out_weight,
    norm_gain,
    expert_ids,
    route_weights,
    gate_weight,
    up_weight,
    down_weight,
    final_gain,
):
    token_count = queries.shape[0]
    query_heads = queries.shape[1] // HEAD_DIM
    key_heads = projected_key_rows.shape[1] // HEAD_DIM
    queries_per_group = query_heads // key_heads
    token_positions = lax.axis_index("sp") * token_count + jnp.arange(token_count, dtype=jnp.int32)
    queries_after_rotation = rotary_over_grid(
        normalize_heads(queries, query_gain, query_heads), token_positions
    ).astype(jnp.bfloat16)
    keys_after_rotation = rotary_over_grid(
        normalize_heads(projected_key_rows, key_norm_gain, key_heads), token_positions
    ).astype(jnp.bfloat16)
    packed = jnp.concatenate(
        [keys_after_rotation, projected_value_rows.reshape(token_count, key_heads, HEAD_DIM)], -1
    ).reshape(token_count, key_heads * 2 * HEAD_DIM)
    grouped_query_heads = (
        queries_after_rotation.reshape(token_count, key_heads, queries_per_group, HEAD_DIM)
        .transpose(1, 2, 0, 3)
        .reshape(key_heads, queries_per_group * token_count, HEAD_DIM)
    )
    score_scale = HEAD_DIM ** (-0.5)
    query_total = queries_per_group * token_count
    group = lax.axis_size("sp")
    section = ring_gather(packed, group, 1 << ((group.bit_length() - 1) // 2)).reshape(
        group * token_count, packed.shape[1]
    )
    running_max = jnp.full((key_heads, query_total), far_below, jnp.float32)
    opened = section.reshape(section.shape[0], key_heads, 2 * HEAD_DIM)
    scores = (
        jnp.einsum(
            "hqd,khd->hqk",
            grouped_query_heads,
            opened[:, :, :HEAD_DIM],
            preferred_element_type=jnp.float32,
        )
        * score_scale
    )
    new_peak = jnp.maximum(running_max, jnp.max(scores, -1))
    weights = jnp.exp(scores - new_peak[:, :, None])
    running_sum = jnp.sum(weights, -1)
    running_out = jnp.einsum(
        "hqk,khd->hqd",
        weights.astype(jnp.bfloat16),
        opened[:, :, HEAD_DIM:],
        preferred_element_type=jnp.float32,
    )
    running_max, running_sum, running_out = (new_peak, running_sum, running_out)
    attended = (running_out / running_sum[:, :, None]).astype(jnp.bfloat16)
    attended = (
        attended.reshape(key_heads, queries_per_group, token_count, HEAD_DIM)
        .transpose(2, 0, 1, 3)
        .reshape(token_count, query_heads * HEAD_DIM)
    )
    expert_count = group
    capacity = 4 * token_count // expert_count
    flat_ids = expert_ids.reshape(-1)
    marked = (flat_ids[:, None] == jnp.arange(expert_count, dtype=jnp.int32)[None, :]).astype(
        jnp.int32
    )
    earlier = jnp.cumsum(marked, 0) - marked
    away = lax.rem(flat_ids - lax.axis_index("sp") + expert_count, expert_count)
    places = (away * capacity + jnp.sum(earlier * marked, 1)).reshape(token_count, TOPK)
    return after_attention(
        attended,
        out_weight,
        residual,
        norm_gain,
        places,
        route_weights,
        gate_weight,
        up_weight,
        down_weight,
        final_gain,
        expert_count,
        lax.axis_size("tp"),
    )


def solution(mesh):
    in_specs = (
        P("sp", "tp"),
        P("sp", "tp"),
        P("sp", "tp"),
        P(),
        P(),
        P("sp", "tp"),
        P("tp", None),
        P("tp"),
        P("sp", None),
        P("sp", None),
        P("sp", None, "tp"),
        P("sp", None, "tp"),
        P("sp", "tp", None),
        P("tp"),
    )
    out_specs = P("sp", "tp")
    return jax.shard_map(
        per_device, mesh=mesh, in_specs=in_specs, out_specs=out_specs, check_vma=False
    )
```

```python
import jax
import jax.numpy as jnp
from jax import lax
from jax.experimental import pallas as pl
from jax.experimental.pallas import tpu as pltpu
from jax.sharding import PartitionSpec as P

D = 2048
HEAD_DIM = 64
GRID_W = 64
TOPK = 2


theta_base = 10000.0
norm_epsilon = 1e-06
residual_scale = 8.0**0.25
far_below = -1e30
MESH = pl.DeviceIdType.MESH


def rope_line(halves, angles):
    pair_count = angles.shape[-1]
    first_half = halves[..., :pair_count]
    second_half = halves[..., pair_count:]
    cosine = jnp.cos(angles)[:, None, :]
    sine_part = jnp.sin(angles)[:, None, :]
    return jnp.concatenate(
        [
            first_half * cosine - second_half * sine_part,
            first_half * sine_part + second_half * cosine,
        ],
        -1,
    )


def rotary_over_grid(rows_by_head, token_positions):
    head_size = rows_by_head.shape[-1]
    frequency = theta_base ** (
        -jnp.arange(0, head_size // 2, 2, dtype=jnp.float32) / (head_size // 2)
    )
    grid_row = (token_positions // GRID_W).astype(jnp.float32)
    grid_col = (token_positions % GRID_W).astype(jnp.float32)
    row_part = rope_line(
        rows_by_head[..., : head_size // 2], grid_row[:, None] * frequency[None, :]
    )
    col_part = rope_line(
        rows_by_head[..., head_size // 2 :], grid_col[:, None] * frequency[None, :]
    )
    return jnp.concatenate([row_part, col_part], -1)


def normalize_heads(token_rows, gain_row, head_count):
    shaped = token_rows.astype(jnp.float32).reshape(token_rows.shape[0], head_count, -1)
    scaled = shaped * lax.rsqrt(jnp.mean(shaped * shaped, -1, keepdims=True) + norm_epsilon)
    return scaled * gain_row[None, None, :]


def ring_gather(packed, group, group_minor):
    rows, width = packed.shape
    pieces = 4
    piece = rows // pieces
    half = group // 2
    major = group // group_minor

    def place_of(index):
        high, low = index // group_minor, lax.rem(index, group_minor)
        if group_minor == 1:
            return high
        back = major - 1 - high
        odd = lax.rem(back, 2)
        inner = (low - 1) * (1 - odd) + (group_minor - 1 - low) * odd
        first = jnp.where(low == 0, 1, 0)
        return first * high + (1 - first) * (major + back * (group_minor - 1) + inner)

    def device_at(place):
        if group_minor == 1:
            return place
        first = jnp.where(place < major, 1, 0)
        rest = jnp.maximum(place - major, 0)
        back = rest // (group_minor - 1)
        inner = lax.rem(rest, group_minor - 1)
        odd = lax.rem(back, 2)
        low = 1 + inner * (1 - odd) + (group_minor - 2 - inner) * odd
        other = (major - 1 - back) * group_minor + low
        return first * (place * group_minor) + (1 - first) * other

    def kernel(mine_ref, all_ref, send_sem, recv_sem, own_sem):
        me = lax.axis_index("sp")
        spot = place_of(me)
        right = device_at(lax.rem(spot + 1, group))
        left = device_at(lax.rem(spot + group - 1, group))
        barrier = pltpu.get_barrier_semaphore()
        for neighbour in (left, right):
            pl.semaphore_signal(
                barrier, inc=1, device_id={"sp": neighbour}, device_id_type=MESH
            )
        pl.semaphore_wait(barrier, 2)
        own = pltpu.make_async_copy(mine_ref, all_ref.at[0], own_sem)
        own.start()
        copies = {}
        for hop in range(1, half + 1):
            for part in range(pieces):
                span = pl.ds(part * piece, piece)
                for way in range(2):
                    if hop == half and (part < pieces // 2) != (way == 0):
                        continue
                    if hop > 1:
                        copies[way, hop - 1, part].wait_recv()
                    source_slot = (hop - 1) if way == 0 else (group - hop + 1)
                    target_slot = hop if way == 0 else group - hop
                    source = mine_ref.at[span] if hop == 1 else all_ref.at[source_slot, span]
                    copy = pltpu.make_async_remote_copy(
                        src_ref=source,
                        dst_ref=all_ref.at[target_slot, span],
                        send_sem=send_sem.at[way, hop - 1, part],
                        recv_sem=recv_sem.at[way, hop - 1, part],
                        device_id={"sp": right if way == 0 else left},
                        device_id_type=MESH,
                    )
                    copy.start()
                    copies[way, hop, part] = copy
        for way, hop, part in copies:
            if hop == half or (hop == half - 1 and (way, half, part) not in copies):
                copies[way, hop, part].wait_recv()
        for copy in copies.values():
            copy.wait_send()
        own.wait()

    return pl.pallas_call(
        kernel,
        out_shape=jax.ShapeDtypeStruct((group, rows, width), packed.dtype),
        in_specs=[pl.BlockSpec(memory_space=pltpu.VMEM)],
        out_specs=pl.BlockSpec(memory_space=pltpu.VMEM),
        scratch_shapes=[
            pltpu.SemaphoreType.DMA((2, half, pieces)),
            pltpu.SemaphoreType.DMA((2, half, pieces)),
            pltpu.SemaphoreType.DMA,
        ],
        compiler_params=pltpu.CompilerParams(
            collective_id=0, has_side_effects=True, vmem_limit_bytes=24 << 20
        ),
    )(packed)


def after_attention(
    attended, out_weight, residual, norm_gain, places, route_weights, gate_weight, up_weight,
    down_weight, final_gain, experts, shards,
):
    token_count, width = residual.shape
    lines = shards // 2
    row_total = TOPK * 2 * token_count
    capacity = row_total // experts
    groups = 4
    group_rows = row_total // groups
    group_experts = experts // groups
    halves = groups
    half_rows = row_total // halves
    hidden_units = gate_weight.shape[2]
    tile = min(256, hidden_units)
    feature_total = width * shards
    places_across = places.T
    bf16, f32 = jnp.bfloat16, jnp.float32

    def kernel(
        att_ref, ow_ref, res_ref, gain_ref, at_ref, across_ref, rw_ref, gate_hbm, up_hbm, down_hbm,
        last_gain_ref, out_ref,
        gate_v, up_v, down_v, weight_sem,
        mix_send, mix_pair, line_send, line_recv, mix_sem, line_sem,
        stat_send, stat_recv, stat_sem,
        outgoing, routed, out_sem, fwd_sem, cross_sem, relay_sem,
        hidden, part_send, part_pair, sum_send, sum_recv, own_sum, other_sum, part_sem, sum_sem,
        result, returned, back_sem,
    ):
        me_s = lax.axis_index("sp")
        me_t = lax.axis_index("tp")
        line = me_t // 2
        core = lax.rem(me_t, 2)
        partner = line * 2 + 1 - core

        def line_at(step):
            return lax.rem(line + step, lines)

        barrier = pltpu.get_barrier_semaphore()
        for step in range(1, experts):
            pl.semaphore_signal(
                barrier, inc=1, device_id={"sp": lax.rem(me_s + step, experts)},
                device_id_type=MESH,
            )
        for step in range(1, shards):
            pl.semaphore_signal(
                barrier, inc=1, device_id={"tp": lax.rem(me_t + step, shards)},
                device_id_type=MESH,
            )
        loads = [
            pltpu.make_async_copy(src.at[0], dst, weight_sem.at[i])
            for i, (src, dst) in enumerate(
                ((gate_hbm, gate_v), (up_hbm, up_v), (down_hbm, down_v))
            )
        ]
        for load in loads:
            load.start()
        sent = []

        def push(source, target, sems, index, device):
            copy = pltpu.make_async_remote_copy(
                src_ref=source, dst_ref=target,
                send_sem=sems.at[(0,) + index], recv_sem=sems.at[(1,) + index],
                device_id=device, device_id_type=MESH,
            )
            copy.start()
            sent.append(copy)
            return copy

        attended_rows = att_ref[...]

        def mix(shard):
            return jnp.dot(
                attended_rows,
                ow_ref[:, pl.ds(pl.multiple_of(shard * width, width), width)],
                preferred_element_type=f32,
            )

        for step in range(lines):
            mix_send[step] = mix(line_at(step) * 2 + 1 - core).astype(bf16)
        pl.semaphore_wait(barrier, experts + shards - 2)
        pair = {}
        for step in list(range(1, lines)) + [0]:
            pair[step] = push(
                mix_send.at[step], mix_pair.at[step], mix_sem, (step,), {"tp": partner}
            )
        across = {}
        for step in range(1, lines):
            mine = mix(line_at(step) * 2 + core)
            pair[step].wait_recv()
            line_send[step - 1] = (mine + mix_pair[step].astype(f32)).astype(bf16)
            across[step] = push(
                line_send.at[step - 1], line_recv.at[step - 1], line_sem, (step - 1,),
                {"tp": line_at(step) * 2 + core},
            )
        total = mix(me_t)
        pair[0].wait_recv()
        total = total + mix_pair[0].astype(f32)
        total = total + residual_scale * res_ref[...].astype(f32)
        for step in range(1, lines):
            across[step].wait_recv()
            total = total + line_recv[step - 1].astype(f32)

        lane = lax.broadcasted_iota(jnp.int32, (token_count, 128), 1)

        def normalize(values, gain, turn):
            sums = jnp.sum(values, 1, keepdims=True)
            squares = jnp.sum(values * values, 1, keepdims=True)
            both = jnp.where(lane == 0, sums, jnp.where(lane == 1, squares, 0.0)).T[:8]
            stat_send[turn] = both
            stats = [
                push(
                    stat_send.at[turn], stat_recv.at[turn, step - 1], stat_sem,
                    (turn, step - 1), {"tp": lax.rem(me_t + step, shards)},
                )
                for step in range(1, shards)
            ]
            for step in range(1, shards):
                stats[step - 1].wait_recv()
                both = both + stat_recv[turn, step - 1]
            columns = jnp.concatenate([both] * 16, 0).T
            center = columns[:, 0:1] / feature_total
            spread = columns[:, 1:2] / feature_total - center * center
            return (values - center) * lax.rsqrt(spread + norm_epsilon) * gain

        normed = normalize(total, gain_ref[...], 0).astype(bf16)
        row_index = lax.broadcasted_iota(jnp.int32, (row_total, token_count), 0)
        picks = jnp.where(
            (row_index == across_ref[0:1, :]) | (row_index == across_ref[1:2, :]), 1.0, 0.0
        ).astype(bf16)
        spread_rows = jnp.dot(picks, normed, preferred_element_type=f32).astype(bf16)
        outgoing[...] = spread_rows
        routed[me_t, pl.ds(0, capacity)] = spread_rows[:capacity]
        arrivals = {}
        for step in range(1, experts):
            rows = pl.ds(step * capacity, capacity)
            arrivals[step] = push(
                outgoing.at[rows], routed.at[me_t, rows], out_sem, (step,),
                {"sp": lax.rem(me_s + step, experts)},
            )
        forwards, crossings, relays = {}, {}, {}

        def forward(group):
            for step in range(group * group_experts, (group + 1) * group_experts):
                if step > 0:
                    arrivals[step].wait_recv()
            rows = pl.ds(group * group_rows, group_rows)
            block = routed.at[me_t, rows]
            for step in range(1, lines):
                crossings[group, step] = push(
                    block, block, cross_sem, (group, step - 1),
                    {"tp": line_at(step) * 2 + core},
                )
            forwards[group] = push(block, block, fwd_sem, (group,), {"tp": partner})

        def relay(group):
            rows = pl.ds(group * group_rows, group_rows)
            for step in range(1, lines):
                crossings[group, step].wait_recv()
                block = routed.at[line_at(lines - step) * 2 + core, rows]
                relays[group, step] = push(
                    block, block, relay_sem, (group, step - 1), {"tp": partner}
                )

        def settle(group):
            forwards[group].wait_recv()
            for step in range(1, lines):
                relays[group, step].wait_recv()

        def expand(half):
            rows = pl.ds(half * half_rows, half_rows)

            def one_tile(index, carry):
                cols = pl.ds(pl.multiple_of(index * tile, tile), tile)
                gate_sum = jnp.zeros((half_rows, tile), f32)
                up_sum = jnp.zeros((half_rows, tile), f32)
                for shard in range(shards):
                    block = routed[shard, rows]
                    deep = pl.ds(shard * width, width)
                    gate_sum += jnp.dot(block, gate_v[deep, cols], preferred_element_type=f32)
                    up_sum += jnp.dot(block, up_v[deep, cols], preferred_element_type=f32)
                hidden[rows, cols] = (
                    gate_sum / (1.0 + jnp.exp(-gate_sum)) * up_sum
                ).astype(bf16)
                return carry

            lax.fori_loop(0, hidden_units // tile, one_tile, 0)

        def down(half, shard):
            return jnp.dot(
                hidden[pl.ds(half * half_rows, half_rows)],
                down_v[:, pl.ds(pl.multiple_of(shard * width, width), width)],
                preferred_element_type=f32,
            )

        parts, sums = {}, {}

        def shrink(half):
            for step in list(range(1, lines)) + [0]:
                part_send[half, step] = down(half, line_at(step) * 2 + 1 - core).astype(bf16)
                parts[half, step] = push(
                    part_send.at[half, step], part_pair.at[half, step], part_sem, (half, step),
                    {"tp": partner},
                )
            for step in range(1, lines):
                other_sum[half, step - 1] = down(half, line_at(step) * 2 + core)
            own_sum[half] = down(half, me_t)

        def join(half):
            for step in range(1, lines):
                parts[half, step].wait_recv()
                sum_send[half, step - 1] = (
                    other_sum[half, step - 1] + part_pair[half, step].astype(f32)
                ).astype(bf16)
                sums[half, step] = push(
                    sum_send.at[half, step - 1], sum_recv.at[half, step - 1], sum_sem,
                    (half, step - 1), {"tp": line_at(step) * 2 + core},
                )

        backs = {}

        def finish(half):
            parts[half, 0].wait_recv()
            value = own_sum[half] + part_pair[half, 0].astype(f32)
            for step in range(1, lines):
                sums[half, step].wait_recv()
                value = value + sum_recv[half, step - 1].astype(f32)
            value = value.astype(bf16)
            result[pl.ds(half * half_rows, half_rows)] = value
            first = half * (experts // halves)
            if half == 0:
                returned[pl.ds(0, capacity)] = value[:capacity]
            for step in range(max(first, 1), first + experts // halves):
                rows = pl.ds(step * capacity, capacity)
                backs[step] = push(
                    result.at[rows], returned.at[rows], back_sem, (step,),
                    {"sp": lax.rem(me_s + experts - step, experts)},
                )

        forward(0)
        forward(1)
        relay(0)
        for load in loads[:2]:
            load.wait()
        settle(0)
        expand(0)
        forward(2)
        relay(1)
        loads[2].wait()
        shrink(0)
        forward(3)
        settle(1)
        join(0)
        expand(1)
        relay(2)
        shrink(1)
        settle(2)
        join(1)
        finish(0)
        expand(2)
        relay(3)
        shrink(2)
        settle(3)
        join(2)
        finish(1)
        expand(3)
        shrink(3)
        join(3)
        finish(2)
        finish(3)
        slot_index = lax.broadcasted_iota(jnp.int32, (token_count, row_total), 1)
        choose = [
            jnp.where(slot_index == at_ref[:, k : k + 1], 1.0, 0.0).astype(bf16)
            for k in range(TOPK)
        ]
        for step in range(1, experts):
            backs[step].wait_recv()
        second_sum = residual_scale * normed.astype(f32)
        back_rows = returned[...]
        for k in range(TOPK):
            second_sum = second_sum + rw_ref[:, k : k + 1] * jnp.dot(
                choose[k], back_rows, preferred_element_type=f32
            )
        out_ref[...] = normalize(second_sum, last_gain_ref[...], 1).astype(bf16)
        for copy in sent:
            copy.wait_send()

    vmem = pl.BlockSpec(memory_space=pltpu.VMEM)
    hbm = pl.BlockSpec(memory_space=pl.ANY)
    dma = pltpu.SemaphoreType.DMA
    other = max(lines - 1, 1)
    return pl.pallas_call(
        kernel,
        out_shape=jax.ShapeDtypeStruct((token_count, width), bf16),
        in_specs=[vmem] * 7 + [hbm] * 3 + [vmem],
        out_specs=vmem,
        scratch_shapes=[
            pltpu.VMEM(gate_weight.shape[1:], bf16),
            pltpu.VMEM(up_weight.shape[1:], bf16),
            pltpu.VMEM(down_weight.shape[1:], bf16),
            dma((3,)),
            pltpu.VMEM((lines, token_count, width), bf16),
            pltpu.VMEM((lines, token_count, width), bf16),
            pltpu.VMEM((other, token_count, width), bf16),
            pltpu.VMEM((other, token_count, width), bf16),
            dma((2, lines)),
            dma((2, other)),
            pltpu.VMEM((2, 8, token_count), f32),
            pltpu.VMEM((2, shards - 1, 8, token_count), f32),
            dma((2, 2, shards - 1)),
            pltpu.VMEM((row_total, width), bf16),
            pltpu.VMEM((shards, row_total, width), bf16),
            dma((2, experts)),
            dma((2, groups)),
            dma((2, groups, other)),
            dma((2, groups, other)),
            pltpu.VMEM((row_total, hidden_units), bf16),
            pltpu.VMEM((halves, lines, half_rows, width), bf16),
            pltpu.VMEM((halves, lines, half_rows, width), bf16),
            pltpu.VMEM((halves, other, half_rows, width), bf16),
            pltpu.VMEM((halves, other, half_rows, width), bf16),
            pltpu.VMEM((halves, half_rows, width), f32),
            pltpu.VMEM((halves, other, half_rows, width), f32),
            dma((2, halves, lines)),
            dma((2, halves, other)),
            pltpu.VMEM((row_total, width), bf16),
            pltpu.VMEM((row_total, width), bf16),
            dma((2, experts)),
        ],
        compiler_params=pltpu.CompilerParams(
            collective_id=1, has_side_effects=True, vmem_limit_bytes=50 << 20
        ),
    )(
        attended, out_weight, residual, norm_gain.reshape(1, -1), places, places_across,
        route_weights, gate_weight, up_weight, down_weight, final_gain.reshape(1, -1),
    )


def per_device(
    queries,
    projected_key_rows,
    projected_value_rows,
    query_gain,
    key_norm_gain,
    residual,
    out_weight,
    norm_gain,
    expert_ids,
    route_weights,
    gate_weight,
    up_weight,
    down_weight,
    final_gain,
):
    token_count = queries.shape[0]
    query_heads = queries.shape[1] // HEAD_DIM
    key_heads = projected_key_rows.shape[1] // HEAD_DIM
    queries_per_group = query_heads // key_heads
    token_positions = lax.axis_index("sp") * token_count + jnp.arange(token_count, dtype=jnp.int32)
    queries_after_rotation = rotary_over_grid(
        normalize_heads(queries, query_gain, query_heads), token_positions
    ).astype(jnp.bfloat16)
    keys_after_rotation = rotary_over_grid(
        normalize_heads(projected_key_rows, key_norm_gain, key_heads), token_positions
    ).astype(jnp.bfloat16)
    packed = jnp.concatenate(
        [keys_after_rotation, projected_value_rows.reshape(token_count, key_heads, HEAD_DIM)], -1
    ).reshape(token_count, key_heads * 2 * HEAD_DIM)
    grouped_query_heads = (
        queries_after_rotation.reshape(token_count, key_heads, queries_per_group, HEAD_DIM)
        .transpose(1, 2, 0, 3)
        .reshape(key_heads, queries_per_group * token_count, HEAD_DIM)
    )
    score_scale = HEAD_DIM ** (-0.5)
    query_total = queries_per_group * token_count
    group = lax.axis_size("sp")
    section = ring_gather(packed, group, 1 << ((group.bit_length() - 1) // 2)).reshape(
        group * token_count, packed.shape[1]
    )
    running_max = jnp.full((key_heads, query_total), far_below, jnp.float32)
    opened = section.reshape(section.shape[0], key_heads, 2 * HEAD_DIM)
    scores = (
        jnp.einsum(
            "hqd,khd->hqk",
            grouped_query_heads,
            opened[:, :, :HEAD_DIM],
            preferred_element_type=jnp.float32,
        )
        * score_scale
    )
    new_peak = jnp.maximum(running_max, jnp.max(scores, -1))
    weights = jnp.exp(scores - new_peak[:, :, None])
    running_sum = jnp.sum(weights, -1)
    running_out = jnp.einsum(
        "hqk,khd->hqd",
        weights.astype(jnp.bfloat16),
        opened[:, :, HEAD_DIM:],
        preferred_element_type=jnp.float32,
    )
    running_max, running_sum, running_out = (new_peak, running_sum, running_out)
    attended = (running_out / running_sum[:, :, None]).astype(jnp.bfloat16)
    attended = (
        attended.reshape(key_heads, queries_per_group, token_count, HEAD_DIM)
        .transpose(2, 0, 1, 3)
        .reshape(token_count, query_heads * HEAD_DIM)
    )
    expert_count = group
    capacity = 4 * token_count // expert_count
    marked = (
        expert_ids[:, :, None] == jnp.arange(expert_count, dtype=jnp.int32)[None, None, :]
    ).astype(jnp.float32)
    token_index = jnp.arange(token_count, dtype=jnp.int32)
    before = (token_index[None, :] < token_index[:, None]).astype(jnp.bfloat16)
    earlier = jnp.dot(
        before, jnp.sum(marked, 1).astype(jnp.bfloat16), preferred_element_type=jnp.float32
    )
    slots = jnp.sum(earlier[:, None, :] * marked, 2).astype(jnp.int32)
    away = lax.rem(expert_ids - lax.axis_index("sp") + expert_count, expert_count)
    places = away * capacity + slots
    return after_attention(
        attended,
        out_weight,
        residual,
        norm_gain,
        places,
        route_weights,
        gate_weight,
        up_weight,
        down_weight,
        final_gain,
        expert_count,
        lax.axis_size("tp"),
    )


def solution(mesh):
    in_specs = (
        P("sp", "tp"),
        P("sp", "tp"),
        P("sp", "tp"),
        P(),
        P(),
        P("sp", "tp"),
        P("tp", None),
        P("tp"),
        P("sp", None),
        P("sp", None),
        P("sp", None, "tp"),
        P("sp", None, "tp"),
        P("sp", "tp", None),
        P("tp"),
    )
    out_specs = P("sp", "tp")
    return jax.shard_map(
        per_device, mesh=mesh, in_specs=in_specs, out_specs=out_specs, check_vma=False
    )
```
